1024 devices in a mesh: sp: 16 (over z), dp: 64 (over y, x, core).
Axes of the slice: x: 4, y: 8, z: 16, core: 2. Of those that a mesh axis runs over, the one named last changes fastest.
Arguments:
- hidden: bfloat16 [64, 2048, 2048], P('dp', 'sp'), may hold values from -6 to 6
- queries: bfloat16 [64, 2048, 1024], P('dp', 'sp'), may hold values from -6 to 6
- values: bfloat16 [64, 2048, 2048], P('dp', 'sp'), may hold values from -6 to 6
- key_weight: bfloat16 [2048, 1024], P('dp'), may hold values from -0.125 to 0.125
- decay_down: bfloat16 [2048, 16], replicated, may hold values from -0.125 to 0.125
- decay_up: float32 [16, 1024], replicated, may hold values from -1.5 to 1.5
- decay_bias: float32 [1024], replicated, may hold values from -1 to 8
- span_shift: bfloat16 [64, 2048], P('dp', 'sp'), may hold values from -1.5 to 1.5, as said below
- norm_gain: float32 [2048], replicated, may hold values from 0.1 to 1.9
Outputs:
- attended: bfloat16 [64, 2048, 2048], P('dp', 'sp')
The draws below stay inside these ranges and needn't reach their ends.
Inputs may be any that keep to these rules, and one draw needn't show every extreme that they name: `span_shift`: constant over each aligned block of 64 positions.
All inputs are finite; a program needn't handle non-finite values.
Results may differ from the reference program's by a relative error of at most 0.0073.
Values may be sent and summed in bfloat16 or wider, within the bound.
A program may use at most 64 MiB of HBM per device.

```python
import jax
import jax.numpy as jnp
from jax import lax

D = 2048
HEADS = 4
DK = 256
DV = 512
RANK = 16
BLOCK = 64
KEY = 1024
VAL = 2048
LENGTH = 2048
BATCH = 64


def draw_decay_bias(key, part):
    pick_key, slow_key, fast_key = jax.random.split(jax.random.fold_in(key, 11), 3)
    share = 5
    slow_pick = jax.random.randint(pick_key, (KEY,), 0, 10) < share
    slow_value = jax.random.uniform(slow_key, (KEY,), jnp.float32, 6.0, 8.0)
    fast_value = jax.random.uniform(fast_key, (KEY,), jnp.float32, -1.0, 0.5)
    return jnp.where(slow_pick, slow_value, fast_value).astype(jnp.float32)


def draw_span_shift(key, part):
    level_key, sign_key = jax.random.split(jax.random.fold_in(key, 23), 2)
    blocks = LENGTH // BLOCK
    levels = jax.random.uniform(level_key, (BATCH, blocks), jnp.float32, -1.5, 1.5)
    return jnp.repeat(levels, BLOCK, axis=1).astype(jnp.bfloat16)


def steps_of(key, shape, cuts, low, top_value):
    loudness, own = 1.0, jax.random.fold_in(key, 6)
    for dim, shards_of in cuts:
        heights = jnp.exp(jax.random.uniform(jax.random.fold_in(own, dim), (shards_of,), jnp.float32, low / len(cuts), top_value / len(cuts)))
        loudness = loudness * jnp.repeat(heights, shape[dim] // shards_of).reshape([-1 if axis == dim else 1 for axis in range(len(shape))])
    return loudness


def gaussian(own_key, shape, spread, reach, cuts=(), dtype=jnp.bfloat16):
    values = jax.random.normal(own_key, shape, jnp.float32) * spread
    if len(cuts) > 0:
        values = steps_of(own_key, shape, cuts, -0.22, 0.18) * values
    return jnp.clip(values, min=-reach, max=reach).astype(dtype)


def setup_inputs(seed: int = 0) -> dict:
    splits = jax.random.split(jax.random.key(seed), 10)
    hidden = gaussian(splits[0], (BATCH, LENGTH, D), 1.0, 6.0, ((0, 64), (1, 16)))
    queries = gaussian(splits[1], (BATCH, LENGTH, KEY), 1.0, 6.0, ((0, 64), (1, 16)))
    values = gaussian(splits[2], (BATCH, LENGTH, VAL), 1.0, 6.0, ((0, 64), (1, 16)))
    key_weight = gaussian(splits[3], (D, KEY), D ** -0.5, 0.125, ((0, 64),))
    decay_down = gaussian(splits[4], (D, RANK), D ** -0.5, 0.125)
    decay_up = gaussian(splits[5], (RANK, KEY), RANK ** -0.5, 1.5, (), jnp.float32)
    decay_bias = draw_decay_bias(jax.random.fold_in(splits[9], 71), 0)
    span_shift = draw_span_shift(jax.random.fold_in(splits[9], 71), 0)
    norm_gain = jnp.clip(1.0 + 0.18 * jax.random.normal(splits[8], (VAL,), jnp.float32), 0.1, 1.9)
    return dict(hidden=hidden, queries=queries, values=values, key_weight=key_weight, decay_down=decay_down, decay_up=decay_up, decay_bias=decay_bias, span_shift=span_shift, norm_gain=norm_gain)


decay_tau = 16.0
norm_eps = 1e-05
highest = lax.Precision.HIGHEST

def mechanism(query, keys_in, value_in, log_decay):
    length, key_width = query.shape
    value_width = value_in.shape[-1]
    blocks = length // BLOCK
    step_decay = log_decay.reshape(blocks, BLOCK, key_width)
    inclusive = jnp.cumsum(step_decay, axis=1)
    exclusive = inclusive - step_decay
    total = inclusive[:, -1, :]
    query3 = query.reshape(blocks, BLOCK, key_width)
    keys3 = keys_in.reshape(blocks, BLOCK, key_width)
    value_tensor3 = value_in.reshape(blocks, BLOCK, value_width)
    query_forward_part = (query3 * jnp.exp(inclusive)).astype(jnp.bfloat16)
    key_fwd = (keys3 * jnp.exp(-inclusive)).astype(jnp.bfloat16)
    query_reverse_part = (query3 * jnp.exp(-exclusive)).astype(jnp.bfloat16)
    key_bwd = (keys3 * jnp.exp(exclusive)).astype(jnp.bfloat16)
    key_end = (keys3 * jnp.exp(total[:, None, :] - inclusive)).astype(jnp.bfloat16)
    fwd_scores = jnp.einsum('nid,njd->nij', query_forward_part, key_fwd, preferred_element_type=jnp.float32)
    bwd_scores = jnp.einsum('nid,njd->nij', query_reverse_part, key_bwd, preferred_element_type=jnp.float32)
    row_index = lax.broadcasted_iota(jnp.int32, (BLOCK, BLOCK), 0)
    col_index = lax.broadcasted_iota(jnp.int32, (BLOCK, BLOCK), 1)
    attention_scores = jnp.where((col_index <= row_index)[None], fwd_scores, bwd_scores).astype(jnp.bfloat16)
    inner_block_term = jnp.einsum('ucy,uyh->uch', attention_scores, value_tensor3, preferred_element_type=jnp.float32)
    end_terms = jnp.einsum('njd,nje->nde', key_end, value_tensor3, preferred_element_type=jnp.float32)
    start_terms = jnp.einsum('njd,nje->nde', key_bwd, value_tensor3, preferred_element_type=jnp.float32)
    rates = jnp.exp(total)

    def forward_step(carry_state, inputs):
        rate, term = inputs
        return (rate[:, None] * carry_state + term, carry_state)

    def backward_step(carry_state, inputs):
        rate, term = inputs
        state_here = rate[:, None] * carry_state
        return (state_here + term, state_here)
    empty = jnp.zeros((key_width, value_width), jnp.float32)
    _, forward_scan_states = lax.scan(forward_step, empty, (rates, end_terms))
    _, reverse_scan_states = lax.scan(backward_step, empty, (rates, start_terms), reverse=True)
    produced_rows = jnp.einsum('tzv,tvg->tzg', query_forward_part, forward_scan_states.astype(jnp.bfloat16), preferred_element_type=jnp.float32)
    produced_rows = produced_rows + jnp.einsum('tzv,tvg->tzg', query_reverse_part, reverse_scan_states.astype(jnp.bfloat16), preferred_element_type=jnp.float32)
    return (inner_block_term + produced_rows).reshape(length, value_width).astype(jnp.bfloat16)

def head_norm(mixed, gain):
    rows = mixed.shape[0]
    grouped = mixed.astype(jnp.float32).reshape(rows, HEADS, DV)
    normed = grouped * lax.rsqrt(lax.optimization_barrier(jnp.mean(grouped * grouped, axis=-1, keepdims=True)) + norm_eps)
    return (normed * gain.reshape(HEADS, DV)[None]).reshape(rows, VAL).astype(jnp.bfloat16)

def reference(hidden, queries, values, key_weight, decay_down, decay_up, decay_bias, span_shift, norm_gain):
    token_rows = hidden.reshape(-1, D)
    keys = jnp.dot(token_rows, key_weight, preferred_element_type=jnp.float32).astype(jnp.bfloat16).reshape(BATCH, LENGTH, KEY)
    low = jnp.dot(token_rows, decay_down, preferred_element_type=jnp.float32).astype(jnp.bfloat16).reshape(BATCH, LENGTH, RANK)

    def per_sequence(inputs):
        query_seq, keys_seq, value_seq, low_seq, shift_seq = inputs
        pre = jnp.dot(low_seq.astype(jnp.float32), decay_up, precision=highest, preferred_element_type=jnp.float32)
        pre = pre + decay_bias[None, :] + shift_seq.astype(jnp.float32)[:, None]
        log_decay = jax.nn.log_sigmoid(pre) / decay_tau

        def by_head(tensor, width):
            return tensor.reshape(LENGTH, HEADS, width).transpose(1, 0, 2)
        scaled = by_head(query_seq, DK).astype(jnp.float32) * DK ** (-0.5)
        mixed = jax.vmap(mechanism)(scaled, by_head(keys_seq, DK).astype(jnp.float32), by_head(value_seq, DV), by_head(log_decay, DK))
        return head_norm(mixed.transpose(1, 0, 2).reshape(LENGTH, VAL), norm_gain)
    return lax.map(per_sequence, (queries, keys, values, low, span_shift))
```

```python
import functools

import jax
import jax.numpy as jnp
from jax import lax
from jax.experimental import pallas as pl
from jax.experimental.pallas import tpu as pltpu
from jax.sharding import Mesh
from jax.sharding import PartitionSpec as P

HEADS = 4
DK = 256
DV = 512
BLOCK = 64
TOK = 128
KEY = 1024
VAL = 2048
DP = ("y", "x", "c")
MESH = pl.DeviceIdType.MESH

GROUPS = 4
ROWS = 32
LAG_NUM, LAG_DEN = 9, 2

decay_tau = 16.0
norm_eps = 1e-05
f32 = jnp.float32
bf16 = jnp.bfloat16
highest = lax.Precision.HIGHEST


def kernel(
    sizes,
    hid_in, q_in, v_in, kw_in, down, up, bias, shift, gain, out,
    hid, q, v, kw, w,
    e1, e2, e3, ends, qf, qb, qe, qF, qB, kf, kb, ke, rate, term, came, went, acc, low,
    in_sem, own_sem, y_send, y_recv, x_send, x_recv, f_send, f_recv, d_send, d_recv,
    s_send, s_recv,
):
    Z, Y, X, C = sizes
    z, y, x, c = (lax.axis_index(a) for a in ("sp", "y", "x", "c"))
    width = KEY // GROUPS
    chunks = KEY // ROWS
    xr, xl, xo = lax.rem(x + 1, X), lax.rem(x + X - 1, X), lax.rem(x + 2, X)
    half = Y // 2

    barrier = pltpu.get_barrier_semaphore()
    peers = [{"y": lax.rem(y + k, Y)} for k in range(1, Y)]
    peers += [{"x": xr}, {"x": xl}, {"c": 1 - c}]
    peers += [{"sp": lax.rem(z + 1, Z)}, {"sp": lax.rem(z + Z - 1, Z)}]
    for peer in peers:
        pl.semaphore_signal(barrier, inc=1, device_id=peer, device_id_type=MESH)

    loads = [
        pltpu.make_async_copy(kw_in, kw, in_sem.at[0]),
        pltpu.make_async_copy(hid_in.at[0], hid, in_sem.at[1]),
        pltpu.make_async_copy(q_in.at[0], q, in_sem.at[2]),
        pltpu.make_async_copy(v_in.at[0], v, in_sem.at[3]),
    ]
    for load in loads:
        load.start()
    owns = [
        pltpu.make_async_copy(kw_in.at[:, pl.ds(g * width, width)], w.at[g, y, x, c], own_sem.at[g])
        for g in range(GROUPS)
    ]
    for own in owns:
        own.start()
    loads[0].wait()
    pl.semaphore_wait(barrier, len(peers))

    def send(src, dst, s, r, peer):
        pltpu.make_async_remote_copy(
            src_ref=src, dst_ref=dst, send_sem=s, recv_sem=r, device_id=peer, device_id_type=MESH
        ).start()

    def wait(ref, sem):
        pltpu.make_async_copy(ref, ref, sem).wait()

    for g in range(GROUPS):
        for k in range(1, Y):
            send(
                kw.at[:, pl.ds(g * width, width)], w.at[g, y, x, c], y_send, y_recv.at[g],
                {"y": lax.rem(y + k, Y)},
            )

    @pl.when(z == 0)
    def _():
        came[0] = jnp.zeros((KEY, DV), bf16)

    @pl.when(z == Z - 1)
    def _():
        came[1] = jnp.zeros((KEY, DV), bf16)

    loads[1].wait()
    low[...] = jnp.dot(hid[...], down[...], preferred_element_type=f32).astype(bf16).astype(f32)
    loads[2].wait()

    row = lax.broadcasted_iota(jnp.int32, (TOK, TOK), 0)
    col = lax.broadcasted_iota(jnp.int32, (TOK, TOK), 1)
    same = (row < BLOCK) == (col < BLOCK)
    upto = jnp.where(same & (row >= col), 1.0, 0.0).astype(f32)
    moved = jnp.transpose(jnp.broadcast_to(shift[...].astype(f32), (TOK, TOK)))
    first = row < BLOCK

    def spread(top, bottom):
        return jnp.where(first, jnp.broadcast_to(top, (TOK, TOK)), jnp.broadcast_to(bottom, (TOK, TOK)))

    @pl.loop(0, KEY // 128)
    def _(j):
        at = pl.ds(pl.multiple_of(j * 128, 128), 128)
        pre = jnp.dot(low[...], up[:, at], precision=highest, preferred_element_type=f32)
        pre = pre + bias[:, at] + moved
        log_decay = (jnp.minimum(pre, 0.0) - jnp.log1p(jnp.exp(-jnp.abs(pre)))) / decay_tau
        inclusive = jnp.dot(upto, log_decay, precision=highest, preferred_element_type=f32)
        exclusive = inclusive - log_decay
        total0, total1 = inclusive[BLOCK - 1 : BLOCK, :], inclusive[TOK - 1 : TOK, :]
        total = spread(total0, total1)
        one = jnp.ones((1, TOK), f32)
        end0, end1 = jnp.exp(total0), jnp.exp(total1)
        ends[0:1, at] = end0
        ends[1:2, at] = end1
        e1[:, at] = jnp.exp(-inclusive)
        e2[:, at] = jnp.exp(exclusive)
        e3[:, at] = jnp.exp(total - inclusive)
        scaled = q[:, at].astype(f32) * DK ** (-0.5)
        forward = scaled * jnp.exp(inclusive)
        reverse = scaled * jnp.exp(total - exclusive)
        qf[:, at] = forward.astype(bf16)
        qb[:, at] = (scaled * jnp.exp(-exclusive)).astype(bf16)
        qe[:, at] = reverse.astype(bf16)
        qF[:, at] = (forward * spread(one, end0)).astype(bf16)
        qB[:, at] = (reverse * spread(end1, one)).astype(bf16)
        rate[at, :] = jnp.transpose(jnp.broadcast_to(end0 * end1, (TOK, TOK)))

    loads[3].wait()

    def after_y(g):
        owns[g].wait()
        wait(w.at[g, pl.ds(0, Y - 1), x, c], y_recv.at[g])
        part = w.at[g, :, x, c]
        send(part, part, x_send.at[0], x_recv.at[0, g], {"x": xr})
        send(part, part, x_send.at[1], x_recv.at[1, g], {"x": xl})
        send(part, part, d_send, d_recv.at[g], {"c": 1 - c})

    def after_x(g):
        for k, (source, target, at) in enumerate(((xl, xr, 0), (xr, xl, half))):
            part = w.at[g, :, source, c]
            wait(part, x_recv.at[k, g])
            piece = w.at[g, pl.ds(at, half), source, c]
            send(piece, piece, f_send.at[k], f_recv.at[k, g], {"x": target})
            send(part, part, d_send, d_recv.at[g], {"c": 1 - c})

    def after_f(g):
        for k, at in enumerate((0, half)):
            wait(w.at[g, pl.ds(at, half), xo, c], f_recv.at[k, g])
        part = w.at[g, :, xo, c]
        send(part, part, d_send, d_recv.at[g], {"c": 1 - c})

    def project(g):
        wait(w.at[g, :, :, 1 - c], d_recv.at[g])
        at = pl.ds(g * width, width)
        head = g * width // DK
        wide = (TOK, width)
        weight = w[g].reshape(Y * X * C * kw.shape[0], width)
        keys = jnp.dot(hid[...], weight, preferred_element_type=f32).astype(bf16).astype(f32)
        rows = lax.broadcasted_iota(jnp.int32, wide, 0) < BLOCK
        end0 = jnp.where(rows, 1.0, jnp.broadcast_to(ends[0:1, at], wide))
        end1 = jnp.where(rows, jnp.broadcast_to(ends[1:2, at], wide), 1.0)
        key_bwd = keys * e2[:, at]
        key_end = keys * e3[:, at]
        kf[:, at] = (keys * e1[:, at]).astype(bf16)
        kb[:, at] = key_bwd.astype(bf16)
        ke[:, at] = key_end.astype(bf16)
        value = v[:, pl.ds(head * DV, DV)]
        over_tokens = (((0,), (0,)), ((), ()))
        term[0, at, :] = lax.dot_general(
            (key_end * end1).astype(bf16), value, over_tokens, preferred_element_type=f32
        )
        term[1, at, :] = lax.dot_general(
            (key_bwd * end0).astype(bf16), value, over_tokens, preferred_element_type=f32
        )

    for s in range(GROUPS + 3):
        for late, stage in enumerate((after_y, after_x, after_f, project)):
            if 0 <= s - late < GROUPS:
                stage(s - late)

    def within(h):
        at = pl.ds(pl.multiple_of(h * DK, DK), DK)
        to = pl.ds(pl.multiple_of(h * DV, DV), DV)
        over_channels = (((1,), (1,)), ((), ()))

        def scores(a, b):
            return lax.dot_general(a[:, at], b[:, at], over_channels, preferred_element_type=f32)

        near = jnp.where(row >= col, scores(qf, kf), scores(qb, kb))
        far = jnp.where(row >= col, scores(qf, ke), scores(qe, kb))
        both = jnp.where(same, near, far).astype(bf16)
        acc[:, to] = jnp.dot(both, v[:, to], preferred_element_type=f32)

    def step(d, n):
        at = pl.ds(pl.multiple_of(n * ROWS, ROWS), ROWS)
        has_prev = jnp.where(d == 0, z > 0, z < Z - 1)
        has_next = jnp.where(d == 0, z < Z - 1, z > 0)
        target = jnp.where(d == 0, lax.rem(z + 1, Z), lax.rem(z + Z - 1, Z))

        @pl.when(has_prev)
        def _():
            wait(came.at[d, at, :], s_recv.at[d, n])

        @pl.when(has_next)
        def _():
            for k in range(DV // 128):
                lanes = pl.ds(k * 128, 128)
                went[d, at, lanes] = (
                    came[d, at, lanes].astype(f32) * rate[at, :] + term[d, at, lanes]
                ).astype(bf16)
            send(went.at[d, at, :], came.at[d, at, :], s_send.at[d], s_recv.at[d, n], {"sp": target})

    early = jnp.where(2 * z < Z, 0, 1)
    apart = jnp.where(2 * z < Z, Z - 1 - 2 * z, 2 * z - (Z - 1))
    lag = jnp.minimum(apart * LAG_NUM // LAG_DEN, chunks)
    at_end = (z == 0) | (z == Z - 1)
    start = jnp.where(at_end, chunks, 0)

    @pl.loop(0, chunks + jnp.maximum(lag, HEADS))
    def _(m):
        @pl.when((m >= start) & (m < start + HEADS))
        def _():
            within(m - start)

        @pl.when(m < chunks)
        def _():
            step(early, m)

        @pl.when((m >= lag) & (m - lag < chunks))
        def _():
            step(1 - early, m - lag)

    @pl.loop(0, HEADS)
    def _(h):
        at = pl.ds(pl.multiple_of(h * DK, DK), DK)
        to = pl.ds(pl.multiple_of(h * DV, DV), DV)
        mixed = acc[:, to] + jnp.dot(qF[:, at], came[0, at, :], preferred_element_type=f32)
        mixed = mixed + jnp.dot(qB[:, at], came[1, at, :], preferred_element_type=f32)
        mixed = mixed.astype(bf16).astype(f32)
        mean = jnp.mean(mixed * mixed, axis=-1, keepdims=True)
        out[0, :, to] = (mixed * lax.rsqrt(mean + norm_eps) * gain[:, to]).astype(bf16)

    wait(w.at[:, pl.ds(0, Y - 1), 0, 0], y_send)
    for k in range(2):
        wait(w.at[:, :, 0, 0], x_send.at[k])
        wait(w.at[:, pl.ds(0, half), 0, 0], f_send.at[k])
    wait(w.at[:, :, :, 0], d_send)

    @pl.when(z < Z - 1)
    def _():
        wait(went.at[0], s_send.at[0])

    @pl.when(z > 0)
    def _():
        wait(went.at[1], s_send.at[1])


def body(sizes, hidden, queries, values, key_weight, decay_down, decay_up, decay_bias, span_shift, norm_gain):
    Z, Y, X, C = sizes
    D = hidden.shape[-1]
    chunks = KEY // ROWS
    hbm = pl.BlockSpec(memory_space=pl.ANY)
    vmem = pl.BlockSpec(memory_space=pltpu.VMEM)
    dma = pltpu.SemaphoreType.DMA
    tokens_by_key = lambda t: pltpu.VMEM((TOK, KEY), t)
    return pl.pallas_call(
        functools.partial(kernel, sizes),
        out_shape=jax.ShapeDtypeStruct((1, TOK, VAL), bf16),
        in_specs=[hbm] * 4 + [vmem] * 5,
        out_specs=vmem,
        scratch_shapes=[
            pltpu.VMEM((TOK, D), bf16),
            pltpu.VMEM((TOK, KEY), bf16),
            pltpu.VMEM((TOK, VAL), bf16),
            pltpu.VMEM(key_weight.shape, bf16),
            pltpu.VMEM((GROUPS, Y, X, C, key_weight.shape[0], KEY // GROUPS), bf16),
            tokens_by_key(f32), tokens_by_key(f32), tokens_by_key(f32),
            pltpu.VMEM((2, KEY), f32),
        ] + [tokens_by_key(bf16)] * 8 + [
            pltpu.VMEM((KEY, 128), f32),
            pltpu.VMEM((2, KEY, DV), f32),
            pltpu.VMEM((2, KEY, DV), bf16),
            pltpu.VMEM((2, KEY, DV), bf16),
            pltpu.VMEM((TOK, VAL), f32),
            pltpu.VMEM((TOK, 16), f32),
            dma((4,)), dma((GROUPS,)), dma, dma((GROUPS,)), dma((2,)), dma((2, GROUPS)),
            dma((2,)), dma((2, GROUPS)), dma, dma((GROUPS,)), dma((2,)), dma((2, chunks)),
        ],
        compiler_params=pltpu.CompilerParams(collective_id=0, has_side_effects=True),
    )(
        hidden, queries, values, key_weight, decay_down, decay_up,
        decay_bias.reshape(1, KEY), span_shift, norm_gain.reshape(1, VAL),
    )


def solution(mesh):
    split = Mesh(mesh.devices.reshape(mesh.shape["sp"], 8, 4, 2), ("sp", "y", "x", "c"))
    return build(split)


def build(split):
    placed = (
        P(DP, "sp", None),
        P(DP, "sp", None),
        P(DP, "sp", None),
        P(DP, None),
        P(),
        P(),
        P(),
        P(DP, "sp"),
        P(),
    )
    sizes = tuple(split.shape[a] for a in ("sp", "y", "x", "c"))
    return jax.shard_map(
        functools.partial(body, sizes),
        mesh=split, in_specs=placed, out_specs=P(DP, "sp", None), check_vma=False,
    )
```

```python
import functools

import jax
import jax.numpy as jnp
from jax import lax
from jax.experimental import pallas as pl
from jax.experimental.pallas import tpu as pltpu
from jax.sharding import Mesh
from jax.sharding import PartitionSpec as P

HEADS = 4
DK = 256
DV = 512
BLOCK = 64
TOK = 128
KEY = 1024
VAL = 2048
DP = ("y", "x", "c")
MESH = pl.DeviceIdType.MESH

GROUPS = 4
ROWS = 16
LAG = 34
PACE = 12

decay_tau = 16.0
norm_eps = 1e-05
f32 = jnp.float32
bf16 = jnp.bfloat16
highest = lax.Precision.HIGHEST


def kernel(
    sizes,
    hid_in, q_in, v_in, kw_in, down, up, bias, shift, gain, out,
    hid, q, v, kw, w,
    e1, e2, e3, ends, qf, qb, qe, qF, qB, kf, kb, ke, rate, term, came, went, acc, low,
    in_sem, own_sem, y_send, y_recv, x_send, x_recv, f_send, f_recv, d_send, d_recv,
    s_send, s_recv, o_sem, res,
):
    Z, Y, X, C = sizes
    z, y, x, c = (lax.axis_index(a) for a in ("sp", "y", "x", "c"))
    width = KEY // GROUPS
    chunks = KEY // ROWS
    xr, xl, xo = lax.rem(x + 1, X), lax.rem(x + X - 1, X), lax.rem(x + 2, X)
    half = Y // 2
    over_channels = (((1,), (1,)), ((), ()))

    barrier = pltpu.get_barrier_semaphore()
    peers = [{"y": lax.rem(y + k, Y)} for k in range(1, Y)]
    peers += [{"x": xr}, {"x": xl}, {"c": 1 - c}]
    peers += [{"sp": lax.rem(z + 1, Z)}, {"sp": lax.rem(z + Z - 1, Z)}]
    for peer in peers:
        pl.semaphore_signal(barrier, inc=1, device_id=peer, device_id_type=MESH)

    loads = [
        pltpu.make_async_copy(kw_in, kw, in_sem.at[0]),
        pltpu.make_async_copy(hid_in.at[0], hid, in_sem.at[1]),
        pltpu.make_async_copy(q_in.at[0], q, in_sem.at[2]),
        pltpu.make_async_copy(v_in.at[0], v, in_sem.at[3]),
    ]
    for load in loads:
        load.start()
    owns = [
        pltpu.make_async_copy(kw_in.at[:, pl.ds(g * width, width)], w.at[g, y, x, c], own_sem.at[g])
        for g in range(GROUPS)
    ]
    for own in owns:
        own.start()
    loads[0].wait()
    pl.semaphore_wait(barrier, len(peers))

    def send(src, dst, s, r, peer):
        pltpu.make_async_remote_copy(
            src_ref=src, dst_ref=dst, send_sem=s, recv_sem=r, device_id=peer, device_id_type=MESH
        ).start()

    def wait(ref, sem):
        pltpu.make_async_copy(ref, ref, sem).wait()

    for g in range(GROUPS):
        for k in range(1, Y):
            send(
                kw.at[:, pl.ds(g * width, width)], w.at[g, y, x, c], y_send, y_recv.at[g],
                {"y": lax.rem(y + k, Y)},
            )

    @pl.when(z == 0)
    def _():
        came[0] = jnp.zeros((KEY, DV), bf16)

    @pl.when(z == Z - 1)
    def _():
        came[1] = jnp.zeros((KEY, DV), bf16)

    loads[1].wait()
    low[...] = (
        lax.dot_general(hid[...], down[...], over_channels, preferred_element_type=f32)
        .astype(bf16)
        .astype(f32)
    )
    loads[2].wait()

    row = lax.broadcasted_iota(jnp.int32, (TOK, TOK), 0)
    col = lax.broadcasted_iota(jnp.int32, (TOK, TOK), 1)
    same = (row < BLOCK) == (col < BLOCK)
    upto = jnp.where(same & (row >= col), 1.0, 0.0).astype(f32)
    moved = jnp.transpose(jnp.broadcast_to(shift[...].astype(f32), (TOK, TOK)))
    first = row < BLOCK

    def spread(top, bottom):
        return jnp.where(first, jnp.broadcast_to(top, (TOK, TOK)), jnp.broadcast_to(bottom, (TOK, TOK)))

    @pl.loop(0, KEY // 128)
    def _(j):
        at = pl.ds(pl.multiple_of(j * 128, 128), 128)
        pre = jnp.dot(low[...], up[:, at], precision=highest, preferred_element_type=f32)
        pre = pre + bias[:, at] + moved
        log_decay = (jnp.minimum(pre, 0.0) - jnp.log1p(jnp.exp(-jnp.abs(pre)))) / decay_tau
        inclusive = jnp.dot(upto, log_decay, precision=highest, preferred_element_type=f32)
        exclusive = inclusive - log_decay
        total0, total1 = inclusive[BLOCK - 1 : BLOCK, :], inclusive[TOK - 1 : TOK, :]
        total = spread(total0, total1)
        one = jnp.ones((1, TOK), f32)
        end0, end1 = jnp.exp(total0), jnp.exp(total1)
        ends[0:1, at] = end0
        ends[1:2, at] = end1
        e1[:, at] = jnp.exp(-inclusive)
        e2[:, at] = jnp.exp(exclusive)
        e3[:, at] = jnp.exp(total - inclusive)
        scaled = q[:, at].astype(f32) * DK ** (-0.5)
        forward = scaled * jnp.exp(inclusive)
        reverse = scaled * jnp.exp(total - exclusive)
        qf[:, at] = forward.astype(bf16)
        qb[:, at] = (scaled * jnp.exp(-exclusive)).astype(bf16)
        qe[:, at] = reverse.astype(bf16)
        qF[:, at] = (forward * spread(one, end0)).astype(bf16)
        qB[:, at] = (reverse * spread(end1, one)).astype(bf16)
        rate[at, :] = jnp.transpose(jnp.broadcast_to(end0 * end1, (TOK, TOK)))

    loads[3].wait()

    def after_y(g):
        owns[g].wait()
        wait(w.at[g, pl.ds(0, Y - 1), x, c], y_recv.at[g])
        part = w.at[g, :, x, c]
        send(part, part, x_send.at[0], x_recv.at[0, g], {"x": xr})
        send(part, part, x_send.at[1], x_recv.at[1, g], {"x": xl})
        send(part, part, d_send, d_recv.at[g], {"c": 1 - c})

    def after_x(g):
        for k, (source, target, at) in enumerate(((xl, xr, 0), (xr, xl, half))):
            part = w.at[g, :, source, c]
            wait(part, x_recv.at[k, g])
            piece = w.at[g, pl.ds(at, half), source, c]
            send(piece, piece, f_send.at[k], f_recv.at[k, g], {"x": target})
            send(part, part, d_send, d_recv.at[g], {"c": 1 - c})

    def after_f(g):
        for k, at in enumerate((0, half)):
            wait(w.at[g, pl.ds(at, half), xo, c], f_recv.at[k, g])
        part = w.at[g, :, xo, c]
        send(part, part, d_send, d_recv.at[g], {"c": 1 - c})

    def project(g):
        wait(w.at[g, :, :, 1 - c], d_recv.at[g])
        at = pl.ds(g * width, width)
        head = g * width // DK
        wide = (TOK, width)
        weight = w[g].reshape(Y * X * C * kw.shape[0], width)
        keys = jnp.dot(hid[...], weight, preferred_element_type=f32).astype(bf16).astype(f32)
        rows = lax.broadcasted_iota(jnp.int32, wide, 0) < BLOCK
        end0 = jnp.where(rows, 1.0, jnp.broadcast_to(ends[0:1, at], wide))
        end1 = jnp.where(rows, jnp.broadcast_to(ends[1:2, at], wide), 1.0)
        key_bwd = keys * e2[:, at]
        key_end = keys * e3[:, at]
        kf[:, at] = (keys * e1[:, at]).astype(bf16)
        kb[:, at] = key_bwd.astype(bf16)
        ke[:, at] = key_end.astype(bf16)
        value = v[:, pl.ds(head * DV, DV)]
        over_tokens = (((0,), (0,)), ((), ()))
        term[0, at, :] = lax.dot_general(
            (key_end * end1).astype(bf16), value, over_tokens, preferred_element_type=f32
        )
        term[1, at, :] = lax.dot_general(
            (key_bwd * end0).astype(bf16), value, over_tokens, preferred_element_type=f32
        )

    def within(h):
        at = pl.ds(pl.multiple_of(h * DK, DK), DK)
        to = pl.ds(pl.multiple_of(h * DV, DV), DV)
        def scores(a, b):
            return lax.dot_general(a[:, at], b[:, at], over_channels, preferred_element_type=f32)

        near = jnp.where(row >= col, scores(qf, kf), scores(qb, kb))
        far = jnp.where(row >= col, scores(qf, ke), scores(qe, kb))
        both = jnp.where(same, near, far).astype(bf16)
        acc[:, to] = jnp.dot(both, v[:, to], preferred_element_type=f32)

    def step(d, n):
        at = pl.ds(pl.multiple_of(n * ROWS, ROWS), ROWS)
        has_prev = jnp.where(d == 0, z > 0, z < Z - 1)
        has_next = jnp.where(d == 0, z < Z - 1, z > 0)
        target = jnp.where(d == 0, lax.rem(z + 1, Z), lax.rem(z + Z - 1, Z))

        @pl.when(has_prev)
        def _():
            wait(came.at[d, at, :], s_recv.at[d, n])

        @pl.when(has_next)
        def _():
            for k in range(DV // 128):
                lanes = pl.ds(k * 128, 128)
                went[d, at, lanes] = (
                    came[d, at, lanes].astype(f32) * rate[at, :] + term[d, at, lanes]
                ).astype(bf16)
            send(went.at[d, at, :], came.at[d, at, :], s_send.at[d], s_recv.at[d, n], {"sp": target})

    def finish(h):
        at = pl.ds(pl.multiple_of(h * DK, DK), DK)
        to = pl.ds(pl.multiple_of(h * DV, DV), DV)
        mixed = acc[:, to] + jnp.dot(qF[:, at], came[0, at, :], preferred_element_type=f32)
        mixed = mixed + jnp.dot(qB[:, at], came[1, at, :], preferred_element_type=f32)
        mixed = mixed.astype(bf16).astype(f32)
        mean = jnp.mean(mixed * mixed, axis=-1, keepdims=True)
        res[:, to] = (mixed * lax.rsqrt(mean + norm_eps) * gain[:, to]).astype(bf16)
        pltpu.make_async_copy(res.at[:, to], out.at[0, :, to], o_sem.at[h]).start()

    early = jnp.where(2 * z < Z, 0, 1)
    edge = jnp.minimum(z, Z - 1 - z)
    per_head = DK // ROWS
    lag = jnp.where(edge == 0, chunks, jnp.minimum((Z - 1 - 2 * edge) * LAG // 4, chunks))

    def before(g):
        part = chunks * g // GROUPS
        return jnp.where(edge == 0, part, jnp.clip(PACE * g - edge * LAG // 4, 0, part))

    start = jnp.where(edge == 0, chunks, before(GROUPS - 1))

    def chain(lo, hi):
        @pl.loop(lo, hi)
        def _(m):
            @pl.when((m >= start) & (m < start + HEADS))
            def _():
                within(m - start)

            @pl.when(m < chunks)
            def _():
                step(early, m)

            n = m - lag

            @pl.when((n >= 0) & (n < chunks))
            def _():
                step(1 - early, n)

                @pl.when(lax.rem(n, per_head) == per_head - 1)
                def _():
                    finish(n // per_head)

    for s in range(GROUPS + 3):
        if s >= 3:
            g = s - 3
            project(g)
            if g < GROUPS - 1:
                chain(before(g), before(g + 1))
        if 0 <= s - 2 < GROUPS:
            after_f(s - 2)
        if 0 <= s - 1 < GROUPS:
            after_x(s - 1)
        if s < GROUPS:
            after_y(s)
    chain(before(GROUPS - 1), chunks + jnp.maximum(lag, HEADS))

    for h in range(HEADS):
        to = pl.ds(h * DV, DV)
        pltpu.make_async_copy(res.at[:, to], out.at[0, :, to], o_sem.at[h]).wait()
    wait(w.at[:, pl.ds(0, Y - 1), 0, 0], y_send)
    for k in range(2):
        wait(w.at[:, :, 0, 0], x_send.at[k])
        wait(w.at[:, pl.ds(0, half), 0, 0], f_send.at[k])
    wait(w.at[:, :, :, 0], d_send)

    @pl.when(z < Z - 1)
    def _():
        wait(went.at[0], s_send.at[0])

    @pl.when(z > 0)
    def _():
        wait(went.at[1], s_send.at[1])


def body(sizes, hidden, queries, values, key_weight, decay_down, decay_up, decay_bias, span_shift, norm_gain):
    Z, Y, X, C = sizes
    D = hidden.shape[-1]
    chunks = KEY // ROWS
    hbm = pl.BlockSpec(memory_space=pl.ANY)
    vmem = pl.BlockSpec(memory_space=pltpu.VMEM)
    dma = pltpu.SemaphoreType.DMA
    tokens_by_key = lambda t: pltpu.VMEM((TOK, KEY), t)
    return pl.pallas_call(
        functools.partial(kernel, sizes),
        out_shape=jax.ShapeDtypeStruct((1, TOK, VAL), bf16),
        in_specs=[hbm] * 4 + [vmem] * 5,
        out_specs=hbm,
        scratch_shapes=[
            pltpu.VMEM((TOK, D), bf16),
            pltpu.VMEM((TOK, KEY), bf16),
            pltpu.VMEM((TOK, VAL), bf16),
            pltpu.VMEM(key_weight.shape, bf16),
            pltpu.VMEM((GROUPS, Y, X, C, key_weight.shape[0], KEY // GROUPS), bf16),
            tokens_by_key(f32), tokens_by_key(f32), tokens_by_key(f32),
            pltpu.VMEM((2, KEY), f32),
        ] + [tokens_by_key(bf16)] * 8 + [
            pltpu.VMEM((KEY, 128), f32),
            pltpu.VMEM((2, KEY, DV), f32),
            pltpu.VMEM((2, KEY, DV), bf16),
            pltpu.VMEM((2, KEY, DV), bf16),
            pltpu.VMEM((TOK, VAL), f32),
            pltpu.VMEM((TOK, 16), f32),
            dma((4,)), dma((GROUPS,)), dma, dma((GROUPS,)), dma((2,)), dma((2, GROUPS)),
            dma((2,)), dma((2, GROUPS)), dma, dma((GROUPS,)), dma((2,)), dma((2, chunks)),
            dma((HEADS,)), pltpu.VMEM((TOK, VAL), bf16),
        ],
        compiler_params=pltpu.CompilerParams(collective_id=0, has_side_effects=True),
    )(
        hidden, queries, values, key_weight, decay_down.T, decay_up,
        decay_bias.reshape(1, KEY), span_shift, norm_gain.reshape(1, VAL),
    )


def solution(mesh):
    split = Mesh(mesh.devices.reshape(mesh.shape["sp"], 8, 4, 2), ("sp", "y", "x", "c"))
    return build(split)


def build(split):
    placed = (
        P(DP, "sp", None),
        P(DP, "sp", None),
        P(DP, "sp", None),
        P(DP, None),
        P(),
        P(),
        P(),
        P(DP, "sp"),
        P(),
    )
    sizes = tuple(split.shape[a] for a in ("sp", "y", "x", "c"))
    return jax.shard_map(
        functools.partial(body, sizes),
        mesh=split, in_specs=placed, out_specs=P(DP, "sp", None), check_vma=False,
    )
```

```python
import functools

import jax
import jax.numpy as jnp
from jax import lax
from jax.experimental import pallas as pl
from jax.experimental.pallas import tpu as pltpu
from jax.sharding import Mesh
from jax.sharding import PartitionSpec as P

HEADS = 4
DK = 256
DV = 512
BLOCK = 64
TOK = 128
KEY = 1024
VAL = 2048
DP = ("y", "x", "c")
MESH = pl.DeviceIdType.MESH

GROUPS = 4
ROWS = 16
LAG = 34
PACE = 12
SKEW = -16

decay_tau = 16.0
norm_eps = 1e-05
f32 = jnp.float32
bf16 = jnp.bfloat16
highest = lax.Precision.HIGHEST


def kernel(
    sizes,
    hid_in, q_in, v_in, kw_in, down, up, bias, shift, gain, out,
    hid, q, v, kw, w,
    e1, e2, e3, ends, qf, qb, qe, qF, qB, kf, kb, ke, rate, term, came, went, acc, low,
    in_sem, own_sem, y_send, y_recv, x_send, x_recv, f_send, f_recv, d_send, d_recv,
    s_send, s_recv, o_sem, res,
):
    Z, Y, X, C = sizes
    z, y, x, c = (lax.axis_index(a) for a in ("sp", "y", "x", "c"))
    width = KEY // GROUPS
    chunks = KEY // ROWS
    xr, xl, xo = lax.rem(x + 1, X), lax.rem(x + X - 1, X), lax.rem(x + 2, X)
    half = Y // 2
    over_channels = (((1,), (1,)), ((), ()))

    barrier = pltpu.get_barrier_semaphore()
    peers = [{"y": lax.rem(y + k, Y)} for k in range(1, Y)]
    peers += [{"x": xr}, {"x": xl}, {"c": 1 - c}]
    peers += [{"sp": lax.rem(z + 1, Z)}, {"sp": lax.rem(z + Z - 1, Z)}]
    for peer in peers:
        pl.semaphore_signal(barrier, inc=1, device_id=peer, device_id_type=MESH)

    loads = [
        pltpu.make_async_copy(kw_in, kw, in_sem.at[0]),
        pltpu.make_async_copy(hid_in.at[0], hid, in_sem.at[1]),
        pltpu.make_async_copy(q_in.at[0], q, in_sem.at[2]),
        pltpu.make_async_copy(v_in.at[0], v, in_sem.at[3]),
    ]
    for load in loads:
        load.start()
    owns = [
        pltpu.make_async_copy(kw_in.at[:, pl.ds(g * width, width)], w.at[g, y, x, c], own_sem.at[g])
        for g in range(GROUPS)
    ]
    for own in owns:
        own.start()
    loads[0].wait()
    pl.semaphore_wait(barrier, len(peers))

    def send(src, dst, s, r, peer):
        pltpu.make_async_remote_copy(
            src_ref=src, dst_ref=dst, send_sem=s, recv_sem=r, device_id=peer, device_id_type=MESH
        ).start()

    def wait(ref, sem):
        pltpu.make_async_copy(ref, ref, sem).wait()

    for g in range(GROUPS):
        for k in range(1, Y):
            send(
                kw.at[:, pl.ds(g * width, width)], w.at[g, y, x, c], y_send, y_recv.at[g],
                {"y": lax.rem(y + k, Y)},
            )

    @pl.when(z == 0)
    def _():
        came[0] = jnp.zeros((KEY, DV), bf16)

    @pl.when(z == Z - 1)
    def _():
        came[1] = jnp.zeros((KEY, DV), bf16)

    loads[1].wait()
    low[...] = (
        lax.dot_general(hid[...], down[...], over_channels, preferred_element_type=f32)
        .astype(bf16)
        .astype(f32)
    )
    loads[2].wait()

    row = lax.broadcasted_iota(jnp.int32, (TOK, TOK), 0)
    col = lax.broadcasted_iota(jnp.int32, (TOK, TOK), 1)
    same = (row < BLOCK) == (col < BLOCK)
    upto = jnp.where(same & (row >= col), 1.0, 0.0).astype(f32)
    moved = jnp.transpose(jnp.broadcast_to(shift[...].astype(f32), (TOK, TOK)))
    first = row < BLOCK

    def spread(top, bottom):
        return jnp.where(first, jnp.broadcast_to(top, (TOK, TOK)), jnp.broadcast_to(bottom, (TOK, TOK)))

    @pl.loop(0, KEY // 128)
    def _(j):
        at = pl.ds(pl.multiple_of(j * 128, 128), 128)
        pre = jnp.dot(low[...], up[:, at], precision=highest, preferred_element_type=f32)
        pre = pre + bias[:, at] + moved
        log_decay = (jnp.minimum(pre, 0.0) - jnp.log1p(jnp.exp(-jnp.abs(pre)))) / decay_tau
        inclusive = jnp.dot(upto, log_decay, precision=highest, preferred_element_type=f32)
        exclusive = inclusive - log_decay
        total0, total1 = inclusive[BLOCK - 1 : BLOCK, :], inclusive[TOK - 1 : TOK, :]
        total = spread(total0, total1)
        one = jnp.ones((1, TOK), f32)
        end0, end1 = jnp.exp(total0), jnp.exp(total1)
        ends[0:1, at] = end0
        ends[1:2, at] = end1
        e1[:, at] = jnp.exp(-inclusive)
        e2[:, at] = jnp.exp(exclusive)
        e3[:, at] = jnp.exp(total - inclusive)
        scaled = q[:, at].astype(f32) * DK ** (-0.5)
        forward = scaled * jnp.exp(inclusive)
        reverse = scaled * jnp.exp(total - exclusive)
        qf[:, at] = forward.astype(bf16)
        qb[:, at] = (scaled * jnp.exp(-exclusive)).astype(bf16)
        qe[:, at] = reverse.astype(bf16)
        qF[:, at] = (forward * spread(one, end0)).astype(bf16)
        qB[:, at] = (reverse * spread(end1, one)).astype(bf16)
        rate[at, :] = jnp.transpose(jnp.broadcast_to(end0 * end1, (TOK, TOK)))

    loads[3].wait()

    def after_y(g):
        owns[g].wait()
        wait(w.at[g, pl.ds(0, Y - 1), x, c], y_recv.at[g])
        part = w.at[g, :, x, c]
        send(part, part, x_send.at[0], x_recv.at[0, g], {"x": xr})
        send(part, part, x_send.at[1], x_recv.at[1, g], {"x": xl})
        send(part, part, d_send, d_recv.at[g], {"c": 1 - c})

    def after_x(g):
        for k, (source, target, at) in enumerate(((xl, xr, 0), (xr, xl, half))):
            part = w.at[g, :, source, c]
            wait(part, x_recv.at[k, g])
            piece = w.at[g, pl.ds(at, half), source, c]
            send(piece, piece, f_send.at[k], f_recv.at[k, g], {"x": target})
            send(part, part, d_send, d_recv.at[g], {"c": 1 - c})

    def after_f(g):
        for k, at in enumerate((0, half)):
            wait(w.at[g, pl.ds(at, half), xo, c], f_recv.at[k, g])
        part = w.at[g, :, xo, c]
        send(part, part, d_send, d_recv.at[g], {"c": 1 - c})

    def project(g):
        wait(w.at[g, :, :, 1 - c], d_recv.at[g])
        at = pl.ds(g * width, width)
        head = g * width // DK
        wide = (TOK, width)
        weight = w[g].reshape(Y * X * C * kw.shape[0], width)
        keys = jnp.dot(hid[...], weight, preferred_element_type=f32).astype(bf16).astype(f32)
        rows = lax.broadcasted_iota(jnp.int32, wide, 0) < BLOCK
        end0 = jnp.where(rows, 1.0, jnp.broadcast_to(ends[0:1, at], wide))
        end1 = jnp.where(rows, jnp.broadcast_to(ends[1:2, at], wide), 1.0)
        key_bwd = keys * e2[:, at]
        key_end = keys * e3[:, at]
        kf[:, at] = (keys * e1[:, at]).astype(bf16)
        kb[:, at] = key_bwd.astype(bf16)
        ke[:, at] = key_end.astype(bf16)
        value = v[:, pl.ds(head * DV, DV)]
        over_tokens = (((0,), (0,)), ((), ()))
        term[0, at, :] = lax.dot_general(
            (key_end * end1).astype(bf16), value, over_tokens, preferred_element_type=f32
        )
        term[1, at, :] = lax.dot_general(
            (key_bwd * end0).astype(bf16), value, over_tokens, preferred_element_type=f32
        )

    def within(h):
        at = pl.ds(pl.multiple_of(h * DK, DK), DK)
        to = pl.ds(pl.multiple_of(h * DV, DV), DV)
        def scores(a, b):
            return lax.dot_general(a[:, at], b[:, at], over_channels, preferred_element_type=f32)

        near = jnp.where(row >= col, scores(qf, kf), scores(qb, kb))
        far = jnp.where(row >= col, scores(qf, ke), scores(qe, kb))
        both = jnp.where(same, near, far).astype(bf16)
        acc[:, to] = jnp.dot(both, v[:, to], preferred_element_type=f32)

    def step(d, n):
        at = pl.ds(pl.multiple_of(n * ROWS, ROWS), ROWS)
        has_prev = jnp.where(d == 0, z > 0, z < Z - 1)
        has_next = jnp.where(d == 0, z < Z - 1, z > 0)
        target = jnp.where(d == 0, lax.rem(z + 1, Z), lax.rem(z + Z - 1, Z))

        @pl.when(has_prev)
        def _():
            wait(came.at[d, at, :], s_recv.at[d, n])

        @pl.when(has_next)
        def _():
            for k in range(DV // 128):
                lanes = pl.ds(k * 128, 128)
                went[d, at, lanes] = (
                    came[d, at, lanes].astype(f32) * rate[at, :] + term[d, at, lanes]
                ).astype(bf16)
            send(went.at[d, at, :], came.at[d, at, :], s_send.at[d], s_recv.at[d, n], {"sp": target})

    def finish(h):
        at = pl.ds(pl.multiple_of(h * DK, DK), DK)
        to = pl.ds(pl.multiple_of(h * DV, DV), DV)
        mixed = acc[:, to] + jnp.dot(qF[:, at], came[0, at, :], preferred_element_type=f32)
        mixed = mixed + jnp.dot(qB[:, at], came[1, at, :], preferred_element_type=f32)
        mixed = mixed.astype(bf16).astype(f32)
        mean = jnp.mean(mixed * mixed, axis=-1, keepdims=True)
        res[:, to] = (mixed * lax.rsqrt(mean + norm_eps) * gain[:, to]).astype(bf16)
        pltpu.make_async_copy(res.at[:, to], out.at[0, :, to], o_sem.at[h]).start()

    ahead = (Z - 1 - 2 * z) * LAG + SKEW * 4
    early = jnp.where(ahead >= 0, 0, 1)
    edge = jnp.where(ahead >= 0, z, Z - 1 - z)
    per_head = DK // ROWS
    lag = jnp.where(edge == 0, chunks, jnp.minimum(jnp.abs(ahead) // 4, chunks))
    far = lag == chunks

    def before(g):
        part = chunks * g // GROUPS
        return jnp.where(edge == 0, part, jnp.clip(PACE * g - edge * LAG // 4, 0, part))

    def chain(lo, hi):
        @pl.loop(lo, hi)
        def _(m):
            @pl.when(far & (m >= chunks) & (m < chunks + HEADS))
            def _():
                within(m - chunks)

            @pl.when(m < chunks)
            def _():
                step(early, m)

            n = m - lag

            @pl.when((n >= 0) & (n < chunks))
            def _():
                step(1 - early, n)

                @pl.when(far & (lax.rem(n, per_head) == per_head - 1))
                def _():
                    finish(n // per_head)

    for s in range(GROUPS + 3):
        if s >= 3:
            g = s - 3
            project(g)
            if g < GROUPS - 1:
                chain(before(g), before(g + 1))

            @pl.when(jnp.logical_not(far))
            def _():
                within(g)

        if 0 <= s - 2 < GROUPS:
            after_f(s - 2)
        if 0 <= s - 1 < GROUPS:
            after_x(s - 1)
        if s < GROUPS:
            after_y(s)
    chain(before(GROUPS - 1), chunks + lag)

    @pl.when(jnp.logical_not(far))
    def _():
        @pl.loop(0, HEADS)
        def _(h):
            finish(h)

    for h in range(HEADS):
        to = pl.ds(h * DV, DV)
        pltpu.make_async_copy(res.at[:, to], out.at[0, :, to], o_sem.at[h]).wait()
    wait(w.at[:, pl.ds(0, Y - 1), 0, 0], y_send)
    for k in range(2):
        wait(w.at[:, :, 0, 0], x_send.at[k])
        wait(w.at[:, pl.ds(0, half), 0, 0], f_send.at[k])
    wait(w.at[:, :, :, 0], d_send)

    @pl.when(z < Z - 1)
    def _():
        wait(went.at[0], s_send.at[0])

    @pl.when(z > 0)
    def _():
        wait(went.at[1], s_send.at[1])


def body(sizes, hidden, queries, values, key_weight, decay_down, decay_up, decay_bias, span_shift, norm_gain):
    Z, Y, X, C = sizes
    D = hidden.shape[-1]
    chunks = KEY // ROWS
    hbm = pl.BlockSpec(memory_space=pl.ANY)
    vmem = pl.BlockSpec(memory_space=pltpu.VMEM)
    dma = pltpu.SemaphoreType.DMA
    tokens_by_key = lambda t: pltpu.VMEM((TOK, KEY), t)
    return pl.pallas_call(
        functools.partial(kernel, sizes),
        out_shape=jax.ShapeDtypeStruct((1, TOK, VAL), bf16),
        in_specs=[hbm] * 4 + [vmem] * 5,
        out_specs=hbm,
        scratch_shapes=[
            pltpu.VMEM((TOK, D), bf16),
            pltpu.VMEM((TOK, KEY), bf16),
            pltpu.VMEM((TOK, VAL), bf16),
            pltpu.VMEM(key_weight.shape, bf16),
            pltpu.VMEM((GROUPS, Y, X, C, key_weight.shape[0], KEY // GROUPS), bf16),
            tokens_by_key(f32), tokens_by_key(f32), tokens_by_key(f32),
            pltpu.VMEM((2, KEY), f32),
        ] + [tokens_by_key(bf16)] * 8 + [
            pltpu.VMEM((KEY, 128), f32),
            pltpu.VMEM((2, KEY, DV), f32),
            pltpu.VMEM((2, KEY, DV), bf16),
            pltpu.VMEM((2, KEY, DV), bf16),
            pltpu.VMEM((TOK, VAL), f32),
            pltpu.VMEM((TOK, 16), f32),
            dma((4,)), dma((GROUPS,)), dma, dma((GROUPS,)), dma((2,)), dma((2, GROUPS)),
            dma((2,)), dma((2, GROUPS)), dma, dma((GROUPS,)), dma((2,)), dma((2, chunks)),
            dma((HEADS,)), pltpu.VMEM((TOK, VAL), bf16),
        ],
        compiler_params=pltpu.CompilerParams(collective_id=0, has_side_effects=True),
    )(
        hidden, queries, values, key_weight, decay_down.T, decay_up,
        decay_bias.reshape(1, KEY), span_shift, norm_gain.reshape(1, VAL),
    )


def solution(mesh):
    split = Mesh(mesh.devices.reshape(mesh.shape["sp"], 8, 4, 2), ("sp", "y", "x", "c"))
    return build(split)


def build(split):
    placed = (
        P(DP, "sp", None),
        P(DP, "sp", None),
        P(DP, "sp", None),
        P(DP, None),
        P(),
        P(),
        P(),
        P(DP, "sp"),
        P(),
    )
    sizes = tuple(split.shape[a] for a in ("sp", "y", "x", "c"))
    return jax.shard_map(
        functools.partial(body, sizes),
        mesh=split, in_specs=placed, out_specs=P(DP, "sp", None), check_vma=False,
    )
```

```python
import functools

import jax
import jax.numpy as jnp
from jax import lax
from jax.experimental import pallas as pl
from jax.experimental.pallas import tpu as pltpu
from jax.sharding import Mesh
from jax.sharding import PartitionSpec as P

HEADS = 4
DK = 256
DV = 512
BLOCK = 64
TOK = 128
KEY = 1024
VAL = 2048
DP = ("y", "x", "c")
MESH = pl.DeviceIdType.MESH

GROUPS = 4
ROWS = 16
LAG = 34
PACE = 12
SKEW = 0

decay_tau = 16.0
norm_eps = 1e-05
f32 = jnp.float32
bf16 = jnp.bfloat16
highest = lax.Precision.HIGHEST


def kernel(
    sizes,
    hid_in, q_in, v_in, kw_in, down, up, bias, shift, gain, out,
    hid, q, v, kw, w,
    e1, e2, e3, ends, qf, qb, qe, qF, qB, kf, kb, ke, rate, term, came, went, acc, low,
    in_sem, own_sem, y_send, y_recv, x_send, x_recv, f_send, f_recv, d_send, d_recv,
    s_send, s_recv, o_sem, res,
):
    Z, Y, X, C = sizes
    z, y, x, c = (lax.axis_index(a) for a in ("sp", "y", "x", "c"))
    width = KEY // GROUPS
    chunks = KEY // ROWS
    xr, xl, xo = lax.rem(x + 1, X), lax.rem(x + X - 1, X), lax.rem(x + 2, X)
    half = Y // 2
    over_channels = (((1,), (1,)), ((), ()))

    barrier = pltpu.get_barrier_semaphore()
    peers = [{"y": lax.rem(y + k, Y)} for k in range(1, Y)]
    peers += [{"x": xr}, {"x": xl}, {"c": 1 - c}]
    for peer in peers:
        pl.semaphore_signal(barrier, inc=1, device_id=peer, device_id_type=MESH)

    @pl.when(z < Z - 1)
    def _():
        pl.semaphore_signal(barrier, inc=1, device_id={"sp": lax.rem(z + 1, Z)}, device_id_type=MESH)

    @pl.when(z > 0)
    def _():
        pl.semaphore_signal(barrier, inc=1, device_id={"sp": lax.rem(z + Z - 1, Z)}, device_id_type=MESH)


    loads = [
        pltpu.make_async_copy(kw_in, kw, in_sem.at[0]),
        pltpu.make_async_copy(hid_in.at[0], hid, in_sem.at[1]),
        pltpu.make_async_copy(q_in.at[0], q, in_sem.at[2]),
        pltpu.make_async_copy(v_in.at[0], v, in_sem.at[3]),
    ]
    for load in loads:
        load.start()
    owns = [
        pltpu.make_async_copy(kw_in.at[:, pl.ds(g * width, width)], w.at[g, y, x, c], own_sem.at[g])
        for g in range(GROUPS)
    ]
    for own in owns:
        own.start()
    loads[0].wait()
    pl.semaphore_wait(barrier, len(peers) + jnp.where((z == 0) | (z == Z - 1), 1, 2))

    def send(src, dst, s, r, peer):
        pltpu.make_async_remote_copy(
            src_ref=src, dst_ref=dst, send_sem=s, recv_sem=r, device_id=peer, device_id_type=MESH
        ).start()

    def wait(ref, sem):
        pltpu.make_async_copy(ref, ref, sem).wait()

    for g in range(GROUPS):
        for k in sorted(range(1, Y), key=lambda k: -min(k, Y - k)):
            send(
                kw.at[:, pl.ds(g * width, width)], w.at[g, y, x, c], y_send, y_recv.at[g],
                {"y": lax.rem(y + k, Y)},
            )

    @pl.when(z == 0)
    def _():
        came[0] = jnp.zeros((KEY, DV), bf16)

    @pl.when(z == Z - 1)
    def _():
        came[1] = jnp.zeros((KEY, DV), bf16)

    loads[1].wait()
    low[...] = (
        lax.dot_general(hid[...], down[...], over_channels, preferred_element_type=f32)
        .astype(bf16)
        .astype(f32)
    )
    loads[2].wait()

    row = lax.broadcasted_iota(jnp.int32, (TOK, TOK), 0)
    col = lax.broadcasted_iota(jnp.int32, (TOK, TOK), 1)
    same = (row < BLOCK) == (col < BLOCK)
    upto = jnp.where(same & (row >= col), 1.0, 0.0).astype(f32)
    moved = jnp.transpose(jnp.broadcast_to(shift[...].astype(f32), (TOK, TOK)))
    first = row < BLOCK

    def spread(top, bottom):
        return jnp.where(first, jnp.broadcast_to(top, (TOK, TOK)), jnp.broadcast_to(bottom, (TOK, TOK)))

    @pl.loop(0, KEY // 128)
    def _(j):
        at = pl.ds(pl.multiple_of(j * 128, 128), 128)
        pre = jnp.dot(low[...], up[:, at], precision=highest, preferred_element_type=f32)
        pre = pre + bias[:, at] + moved
        log_decay = (jnp.minimum(pre, 0.0) - jnp.log1p(jnp.exp(-jnp.abs(pre)))) / decay_tau
        inclusive = jnp.dot(upto, log_decay, precision=highest, preferred_element_type=f32)
        exclusive = inclusive - log_decay
        total0, total1 = inclusive[BLOCK - 1 : BLOCK, :], inclusive[TOK - 1 : TOK, :]
        total = spread(total0, total1)
        one = jnp.ones((1, TOK), f32)
        end0, end1 = jnp.exp(total0), jnp.exp(total1)
        ends[0:1, at] = end0
        ends[1:2, at] = end1
        e1[:, at] = jnp.exp(-inclusive)
        e2[:, at] = jnp.exp(exclusive)
        e3[:, at] = jnp.exp(total - inclusive)
        scaled = q[:, at].astype(f32) * DK ** (-0.5)
        forward = scaled * jnp.exp(inclusive)
        reverse = scaled * jnp.exp(total - exclusive)
        qf[:, at] = forward.astype(bf16)
        qb[:, at] = (scaled * jnp.exp(-exclusive)).astype(bf16)
        qe[:, at] = reverse.astype(bf16)
        qF[:, at] = (forward * spread(one, end0)).astype(bf16)
        qB[:, at] = (reverse * spread(end1, one)).astype(bf16)
        rate[at, :] = jnp.transpose(jnp.broadcast_to(end0 * end1, (TOK, TOK)))

    loads[3].wait()

    def after_y(g):
        owns[g].wait()
        wait(w.at[g, pl.ds(0, Y - 1), x, c], y_recv.at[g])
        part = w.at[g, :, x, c]
        send(part, part, x_send.at[0], x_recv.at[0, g], {"x": xr})
        send(part, part, x_send.at[1], x_recv.at[1, g], {"x": xl})
        send(part, part, d_send, d_recv.at[g], {"c": 1 - c})

    def after_x(g):
        for k, (source, target, at) in enumerate(((xl, xr, 0), (xr, xl, half))):
            part = w.at[g, :, source, c]
            wait(part, x_recv.at[k, g])
            piece = w.at[g, pl.ds(at, half), source, c]
            send(piece, piece, f_send.at[k], f_recv.at[k, g], {"x": target})
            send(part, part, d_send, d_recv.at[g], {"c": 1 - c})

    def after_f(g):
        for k, at in enumerate((0, half)):
            wait(w.at[g, pl.ds(at, half), xo, c], f_recv.at[k, g])
        part = w.at[g, :, xo, c]
        send(part, part, d_send, d_recv.at[g], {"c": 1 - c})

    def project(g):
        wait(w.at[g, :, :, 1 - c], d_recv.at[g])
        at = pl.ds(g * width, width)
        head = g * width // DK
        wide = (TOK, width)
        weight = w[g].reshape(Y * X * C * kw.shape[0], width)
        keys = jnp.dot(hid[...], weight, preferred_element_type=f32).astype(bf16).astype(f32)
        rows = lax.broadcasted_iota(jnp.int32, wide, 0) < BLOCK
        end0 = jnp.where(rows, 1.0, jnp.broadcast_to(ends[0:1, at], wide))
        end1 = jnp.where(rows, jnp.broadcast_to(ends[1:2, at], wide), 1.0)
        key_bwd = keys * e2[:, at]
        key_end = keys * e3[:, at]
        kf[:, at] = (keys * e1[:, at]).astype(bf16)
        kb[:, at] = key_bwd.astype(bf16)
        ke[:, at] = key_end.astype(bf16)
        value = v[:, pl.ds(head * DV, DV)]
        over_tokens = (((0,), (0,)), ((), ()))
        term[0, at, :] = lax.dot_general(
            (key_end * end1).astype(bf16), value, over_tokens, preferred_element_type=f32
        )
        term[1, at, :] = lax.dot_general(
            (key_bwd * end0).astype(bf16), value, over_tokens, preferred_element_type=f32
        )

    def within(h):
        at = pl.ds(pl.multiple_of(h * DK, DK), DK)
        to = pl.ds(pl.multiple_of(h * DV, DV), DV)
        def scores(a, b):
            return lax.dot_general(a[:, at], b[:, at], over_channels, preferred_element_type=f32)

        near = jnp.where(row >= col, scores(qf, kf), scores(qb, kb))
        far = jnp.where(row >= col, scores(qf, ke), scores(qe, kb))
        both = jnp.where(same, near, far).astype(bf16)
        acc[:, to] = jnp.dot(both, v[:, to], preferred_element_type=f32)

    def step(d, n):
        at = pl.ds(pl.multiple_of(n * ROWS, ROWS), ROWS)
        has_prev = jnp.where(d == 0, z > 0, z < Z - 1)
        has_next = jnp.where(d == 0, z < Z - 1, z > 0)
        target = jnp.where(d == 0, lax.rem(z + 1, Z), lax.rem(z + Z - 1, Z))

        @pl.when(has_prev)
        def _():
            wait(came.at[d, at, :], s_recv.at[d, n])

        @pl.when(has_next)
        def _():
            for k in range(DV // 128):
                lanes = pl.ds(k * 128, 128)
                went[d, at, lanes] = (
                    came[d, at, lanes].astype(f32) * rate[at, :] + term[d, at, lanes]
                ).astype(bf16)
            send(went.at[d, at, :], came.at[d, at, :], s_send.at[d], s_recv.at[d, n], {"sp": target})

    def finish(h):
        at = pl.ds(pl.multiple_of(h * DK, DK), DK)
        to = pl.ds(pl.multiple_of(h * DV, DV), DV)
        mixed = acc[:, to] + jnp.dot(qF[:, at], came[0, at, :], preferred_element_type=f32)
        mixed = mixed + jnp.dot(qB[:, at], came[1, at, :], preferred_element_type=f32)
        mixed = mixed.astype(bf16).astype(f32)
        mean = jnp.mean(mixed * mixed, axis=-1, keepdims=True)
        res[:, to] = (mixed * lax.rsqrt(mean + norm_eps) * gain[:, to]).astype(bf16)
        pltpu.make_async_copy(res.at[:, to], out.at[0, :, to], o_sem.at[h]).start()

    ahead = (Z - 1 - 2 * z) * LAG + SKEW * 4
    early = jnp.where(ahead >= 0, 0, 1)
    edge = jnp.where(ahead >= 0, z, Z - 1 - z)
    per_head = DK // ROWS
    lag = jnp.where(edge == 0, chunks, jnp.minimum(jnp.abs(ahead) // 4, chunks))
    far = lag == chunks

    def before(g):
        part = chunks * g // GROUPS
        return jnp.where(edge == 0, part, jnp.clip(PACE * g - edge * LAG // 4, 0, part))

    def chain(lo, hi):
        @pl.loop(lo, hi)
        def _(m):
            @pl.when(far & (m >= chunks) & (m < chunks + HEADS))
            def _():
                within(m - chunks)

            @pl.when(m < chunks)
            def _():
                step(early, m)

            n = m - lag

            @pl.when((n >= 0) & (n < chunks))
            def _():
                step(1 - early, n)

                @pl.when(far & (lax.rem(n, per_head) == per_head - 1))
                def _():
                    finish(n // per_head)

    for s in range(GROUPS + 3):
        if s >= 3:
            g = s - 3
            project(g)
            if g < GROUPS - 1:
                chain(before(g), before(g + 1))

            @pl.when(jnp.logical_not(far))
            def _():
                within(g)

        if 0 <= s - 2 < GROUPS:
            after_f(s - 2)
        if 0 <= s - 1 < GROUPS:
            after_x(s - 1)
        if s < GROUPS:
            after_y(s)
    chain(before(GROUPS - 1), chunks + lag)

    @pl.when(jnp.logical_not(far))
    def _():
        @pl.loop(0, HEADS)
        def _(h):
            finish(h)

    for h in range(HEADS):
        to = pl.ds(h * DV, DV)
        pltpu.make_async_copy(res.at[:, to], out.at[0, :, to], o_sem.at[h]).wait()
    wait(w.at[:, pl.ds(0, Y - 1), 0, 0], y_send)
    for k in range(2):
        wait(w.at[:, :, 0, 0], x_send.at[k])
        wait(w.at[:, pl.ds(0, half), 0, 0], f_send.at[k])
    wait(w.at[:, :, :, 0], d_send)

    @pl.when(z < Z - 1)
    def _():
        wait(went.at[0], s_send.at[0])

    @pl.when(z > 0)
    def _():
        wait(went.at[1], s_send.at[1])


def body(sizes, hidden, queries, values, key_weight, decay_down, decay_up, decay_bias, span_shift, norm_gain):
    Z, Y, X, C = sizes
    D = hidden.shape[-1]
    chunks = KEY // ROWS
    hbm = pl.BlockSpec(memory_space=pl.ANY)
    vmem = pl.BlockSpec(memory_space=pltpu.VMEM)
    dma = pltpu.SemaphoreType.DMA
    tokens_by_key = lambda t: pltpu.VMEM((TOK, KEY), t)
    return pl.pallas_call(
        functools.partial(kernel, sizes),
        out_shape=jax.ShapeDtypeStruct((1, TOK, VAL), bf16),
        in_specs=[hbm] * 4 + [vmem] * 5,
        out_specs=hbm,
        scratch_shapes=[
            pltpu.VMEM((TOK, D), bf16),
            pltpu.VMEM((TOK, KEY), bf16),
            pltpu.VMEM((TOK, VAL), bf16),
            pltpu.VMEM(key_weight.shape, bf16),
            pltpu.VMEM((GROUPS, Y, X, C, key_weight.shape[0], KEY // GROUPS), bf16),
            tokens_by_key(f32), tokens_by_key(f32), tokens_by_key(f32),
            pltpu.VMEM((2, KEY), f32),
        ] + [tokens_by_key(bf16)] * 8 + [
            pltpu.VMEM((KEY, 128), f32),
            pltpu.VMEM((2, KEY, DV), f32),
            pltpu.VMEM((2, KEY, DV), bf16),
            pltpu.VMEM((2, KEY, DV), bf16),
            pltpu.VMEM((TOK, VAL), f32),
            pltpu.VMEM((TOK, 16), f32),
            dma((4,)), dma((GROUPS,)), dma, dma((GROUPS,)), dma((2,)), dma((2, GROUPS)),
            dma((2,)), dma((2, GROUPS)), dma, dma((GROUPS,)), dma((2,)), dma((2, chunks)),
            dma((HEADS,)), pltpu.VMEM((TOK, VAL), bf16),
        ],
        compiler_params=pltpu.CompilerParams(collective_id=0, has_side_effects=True),
    )(
        hidden, queries, values, key_weight, decay_down.T, decay_up,
        decay_bias.reshape(1, KEY), span_shift, norm_gain.reshape(1, VAL),
    )


def solution(mesh):
    split = Mesh(mesh.devices.reshape(mesh.shape["sp"], 8, 4, 2), ("sp", "y", "x", "c"))
    return build(split)


def build(split):
    placed = (
        P(DP, "sp", None),
        P(DP, "sp", None),
        P(DP, "sp", None),
        P(DP, None),
        P(),
        P(),
        P(),
        P(DP, "sp"),
        P(),
    )
    sizes = tuple(split.shape[a] for a in ("sp", "y", "x", "c"))
    return jax.shard_map(
        functools.partial(body, sizes),
        mesh=split, in_specs=placed, out_specs=P(DP, "sp", None), check_vma=False,
    )
```
